32 devices in a mesh: sp: 8 (over z, x), tp: 4 (over y, core).
Axes of the slice: x: 2, y: 2, z: 4, core: 2. Of those that a mesh axis runs over, the one named last changes fastest.
Arguments:
- residual_in: bfloat16 [1536, 2048], P('sp', 'tp'), may hold values from -6 to 6
- query_rows: bfloat16 [1536, 1024], P('sp', 'tp'), may hold values from -8 to 8
- key_rows: bfloat16 [1536, 1024], P('sp', 'tp'), may hold values from -8 to 8
- value_rows: bfloat16 [1536, 1024], P('sp', 'tp'), may hold values from -6 to 6
- map_weight: float32 [16], P('tp'), may hold values from 0.3 to 0.8
- head_gain: float32 [64], replicated, may hold values from 0.1 to 1.9
- out_proj: bfloat16 [1024, 2048], P(None, 'tp'), may hold values from -0.1875 to 0.1875
- norm_gain: float32 [2048], replicated, may hold values from 0.1 to 1.9
- route_ids: int32 [1536, 2], P('sp'), may hold values from 0 to 7, all different within a row; in each aligned block of 192 rows (0 to 191, 192 to 383, ...) at most 60 rows name the same one
- route_weights: float32 [1536, 2], P('sp'), may hold values from 0.2 to 1.2
- expert_gate: bfloat16 [8, 1024, 2048], P('sp', 'tp'), may hold values from -0.125 to 0.125
- expert_up: bfloat16 [8, 1024, 2048], P('sp', 'tp'), may hold values from -0.125 to 0.125
- expert_down: bfloat16 [8, 1024, 2048], P('sp', None, 'tp'), may hold values from -0.1875 to 0.1875
- shared_gate: bfloat16 [1024, 2048], P('tp'), may hold values from -0.125 to 0.125
- shared_up: bfloat16 [1024, 2048], P('tp'), may hold values from -0.125 to 0.125
- shared_down: bfloat16 [1024, 2048], P(None, 'tp'), may hold values from -0.1875 to 0.1875
Outputs:
- mixed_out: bfloat16 [1536, 2048], P('sp', 'tp')
The draws below stay inside these ranges and needn't reach their ends.
Inputs may be any that keep to these rules, and one draw needn't show every extreme that they name: `route_ids`: each row names 2 different experts. Among the rows held by one index of sp no expert is named more than 60 times, and in every draw some expert is named exactly 60 times by the rows of some index of sp.
All inputs are finite; a program needn't handle non-finite values.
Results may differ from the reference program's by a relative error of at most 0.0095.
Values may be sent and summed in bfloat16 or wider, within the bound.
No kernel may reach another device: no remote copies, remote signals or barrier semaphores. Data moves between devices by JAX's collectives and lax.ppermute only.
A program may use at most 64 MiB of HBM per device.

```python
import math
from functools import partial
import jax
import jax.numpy as jnp
import numpy as np
from jax import lax

D = 2048
H = 16
HD = 64
FE = 1024
TOPK = 2
SEQ_DEV = 192
TOKENS = 1536
EXPERTS = 8
CAPACITY = 60
N_SP = 8


def query_key_pair(key):
    query_key = jax.random.fold_in(key, 11)
    second_key = jax.random.fold_in(key, 12)
    full_shape = (TOKENS, H * HD)
    queries = jnp.clip(jax.random.normal(query_key, full_shape, jnp.float32) * 1.3, -8.0, 8.0)
    key_vals = jnp.clip(jax.random.normal(second_key, full_shape, jnp.float32) * 1.3, -8.0, 8.0)
    return (queries, key_vals)


def draw_query_rows(key, part):
    return query_key_pair(key)[0].astype(jnp.bfloat16)


def draw_key_rows(key, part):
    return query_key_pair(key)[1].astype(jnp.bfloat16)


def block_scale(rng, extent, pieces, low, high):
    def one(dim, shards_of):
        heights = jax.random.uniform(jax.random.fold_in(jax.random.fold_in(rng, 6), dim), (shards_of,), jnp.float32, low / len(pieces), high / len(pieces))
        return jnp.repeat(jnp.exp(heights), extent[dim] // shards_of).reshape((-1,) + (1,) * (len(extent) - dim - 1))

    loudness = one(*pieces[0])
    for cut in pieces[1:]:
        loudness = loudness * one(*cut)
    return loudness


def deal_out(rng, own, number, rows, number_of, top, reach, slope):
    ranking = jax.random.permutation(rng, number_of)
    packed, usual = shares(number_of, rows * top, reach, slope, True), shares(number_of, rows * top, reach, slope, False)
    places = jnp.arange(number_of)

    def named(lengths, rotation):
        used = int((lengths > 0).sum())
        fixed = max(1, used // 4)
        passed = fixed + (places - fixed + rotation * (used - fixed)) % max(1, number_of - fixed)
        return jnp.zeros((number_of,), jnp.int32).at[ranking[jnp.where(places < fixed, places, passed)]].set(jnp.asarray(lengths, jnp.int32))

    lengths = jnp.where(number % 4 == 0, named(packed, number // 4), named(usual, number - number // 4 - 1))
    mixed = jax.random.permutation(jax.random.fold_in(own, 3), number_of)
    donor, receiver = mixed[0:number_of // 2 * 2:2], mixed[1:number_of // 2 * 2:2]
    slack = jnp.minimum(lengths[donor] - 1, reach - lengths[receiver]) // 2
    slack = jnp.where((donor == ranking[0]) | (receiver == ranking[0]) | (lengths[receiver] == 0), 0, jnp.maximum(slack, 0))
    passed = jax.random.randint(jax.random.fold_in(own, 4), (number_of // 2,), 0, 1 << 20) % (slack + 1)
    lengths = lengths.at[donor].add(-passed).at[receiver].add(passed)
    items = jnp.searchsorted(jnp.cumsum(lengths), jnp.arange(rows * top), side="right").astype(jnp.int32)
    listing = items.reshape(top, rows).T
    listing = listing[jax.random.permutation(jax.random.fold_in(own, 1), rows)]
    rotation = jax.random.randint(jax.random.fold_in(own, 2), (rows, 1), 0, top)
    return jnp.take_along_axis(listing, (jnp.arange(top)[None, :] + rotation) % top, axis=1)


def shares(amount, total, most, skew, full):
    loads = [(1 << 20) // math.isqrt(grade ** skew) + 1 for grade in range(1, amount + 1)]
    largest = most if full else min(most, max(-(-total // amount), total * loads[0] // sum(loads)))
    least = 1 if total - largest >= amount - 1 else 0
    given, rest = [largest] + [least] * (amount - 1), total - largest - least * (amount - 1)
    while rest > 0:
        movable = [i for i in range(1, amount) if given[i] < largest] or [i for i in range(1, amount) if given[i] < most]
        mass, remaining = sum([loads[i] for i in movable]), rest
        for i in movable:
            extra = min(most - given[i], max(1, remaining * loads[i] // mass), rest)
            given[i] = given[i] + extra
            rest = rest - extra
    return np.array(given)


def gaussian(rng, extent, spread, reach, cuts=(), kind=jnp.bfloat16):
    entries = spread * jax.random.normal(rng, extent, jnp.float32)
    if cuts:
        entries = entries * block_scale(rng, extent, cuts, -0.22, 0.18)
    return jnp.clip(entries, -reach, reach).astype(kind)


def setup_inputs(seed: int = 0) -> dict:
    seeds = jax.random.split(jax.random.key(seed), 17)
    residual_in = gaussian(seeds[0], (TOKENS, D), 1.0, 6.0, ((0, 8), (1, 4)))
    query_rows = draw_query_rows(jax.random.fold_in(seeds[16], 71), 0)
    key_rows = draw_key_rows(jax.random.fold_in(seeds[16], 71), 0)
    value_rows = gaussian(seeds[3], (TOKENS, H * HD), 1.0, 6.0, ((0, 8), (1, 4)))
    map_weight = jnp.clip(0.3 + 0.5 * jax.random.uniform(seeds[4], (H,), jnp.float32) ** block_scale(seeds[4], (H,), ((0, 4),), -0.2, 0.2), 0.3, 0.8)
    head_gain = jnp.clip(1.0 + 0.18 * jax.random.normal(seeds[5], (HD,), jnp.float32), 0.1, 1.9)
    out_proj = gaussian(seeds[6], (H * HD, D), (H * HD) ** -0.5, 0.1875, ((1, 4),))
    norm_gain = jnp.clip(1.0 + 0.18 * jax.random.normal(seeds[7], (D,), jnp.float32), 0.1, 1.9)
    route_ids_keys = jax.random.split(jax.random.fold_in(seeds[8], 1), TOKENS // SEQ_DEV)
    route_ids_turns = jax.random.permutation(jax.random.fold_in(seeds[8], 3), TOKENS // SEQ_DEV)
    route_ids = jax.vmap(lambda own, number: deal_out(jax.random.fold_in(seeds[8], 2), own, number, SEQ_DEV, EXPERTS, TOPK, CAPACITY, 2))(route_ids_keys, route_ids_turns).reshape((TOKENS, TOPK))
    route_weights = jnp.clip(0.2 + 1 * jax.random.uniform(seeds[9], (TOKENS, TOPK), jnp.float32) ** block_scale(seeds[9], (TOKENS, TOPK), ((0, 8),), -0.2, 0.2), 0.2, 1.2)
    expert_gate = gaussian(seeds[10], (EXPERTS, FE, D), D ** -0.5, 0.125, ((0, 8), (1, 4)))
    expert_up = gaussian(seeds[11], (EXPERTS, FE, D), D ** -0.5, 0.125, ((0, 8), (1, 4)))
    expert_down = gaussian(seeds[12], (EXPERTS, FE, D), FE ** -0.5, 0.1875, ((0, 8), (2, 4)))
    shared_gate = gaussian(seeds[13], (FE, D), D ** -0.5, 0.125, ((0, 4),))
    shared_up = gaussian(seeds[14], (FE, D), D ** -0.5, 0.125, ((0, 4),))
    shared_down = gaussian(seeds[15], (FE, D), FE ** -0.5, 0.1875, ((1, 4),))
    return {"residual_in": residual_in, "query_rows": query_rows, "key_rows": key_rows, "value_rows": value_rows, "map_weight": map_weight, "head_gain": head_gain, "out_proj": out_proj, "norm_gain": norm_gain, "route_ids": route_ids, "route_weights": route_weights, "expert_gate": expert_gate, "expert_up": expert_up, "expert_down": expert_down, "shared_gate": shared_gate, "shared_up": shared_up, "shared_down": shared_down}


epsilon = 1e-06
masked_score = -1e+30

def rms_scale(values, gain_vec):
    squares = lax.optimization_barrier(jnp.mean(values * values, axis=-1, keepdims=True))
    return values * lax.rsqrt(squares + epsilon) * gain_vec

def block_slots(route_block, experts_all, capacity):
    flat_ids = route_block.reshape(-1)
    one_hot = (flat_ids[:, None] == jnp.arange(experts_all, dtype=jnp.int32)[None, :]).astype(jnp.int32)
    earlier = jnp.cumsum(one_hot, axis=0) - one_hot
    position = lax.optimization_barrier(jnp.sum(earlier * one_hot, axis=1))
    return (flat_ids * capacity + position).astype(jnp.int32).reshape(route_block.shape)

def reference(residual_in, query_rows, key_rows, value_rows, map_weight, head_gain, out_proj, norm_gain, route_ids, route_weights, expert_gate, expert_up, expert_down, shared_gate, shared_up, shared_down):
    half_dim = HD // 2
    block_len = min(256, TOKENS)
    block_count = TOKENS // block_len
    key_heads = key_rows.reshape(TOKENS, H, 2, half_dim).astype(jnp.float32)
    value_heads = value_rows.reshape(TOKENS, H, HD).astype(jnp.float32)
    query_blocks = query_rows.reshape(block_count, block_len, H, 2, half_dim)
    key_pos = jnp.arange(TOKENS, dtype=jnp.int32)

    def attend(operands):
        query_block, block_index = operands
        query_pos = block_index * block_len + jnp.arange(block_len, dtype=jnp.int32)
        scores = jnp.einsum('qhmd,khmd->mhqk', query_block.astype(jnp.float32), key_heads) * half_dim ** (-0.5)
        visible = key_pos[None, :] <= query_pos[:, None]
        scores = jnp.where(visible, scores, masked_score)
        row_max = lax.optimization_barrier(jnp.max(scores, axis=-1, keepdims=True))
        expo = jnp.where(visible, jnp.exp(scores - row_max), 0.0)
        totals = lax.optimization_barrier(jnp.sum(expo, axis=-1))
        rounded = lax.optimization_barrier(expo.astype(jnp.bfloat16)).astype(jnp.float32)
        summed = jnp.einsum('mhqk,khd->mhqd', rounded, value_heads) / totals[..., None]
        return summed[0] - map_weight[:, None, None] * summed[1]
    parts = lax.map(attend, (query_blocks, jnp.arange(block_count, dtype=jnp.int32)))
    head_out = rms_scale(parts, head_gain).astype(jnp.bfloat16)
    head_out = jnp.transpose(head_out, (0, 2, 1, 3)).reshape(TOKENS, H * HD)
    attn = jnp.dot(head_out, out_proj, preferred_element_type=jnp.float32)
    hidden_state = (residual_in.astype(jnp.float32) + attn).astype(jnp.bfloat16)
    normed = rms_scale(hidden_state.astype(jnp.float32), norm_gain).astype(jnp.bfloat16)
    shared_hidden = (jax.nn.silu(jnp.dot(normed, shared_gate.T, preferred_element_type=jnp.float32)) * jnp.dot(normed, shared_up.T, preferred_element_type=jnp.float32)).astype(jnp.bfloat16)
    shared_out = jnp.dot(shared_hidden, shared_down, preferred_element_type=jnp.float32)
    slot_ids = jax.vmap(partial(block_slots, experts_all=EXPERTS, capacity=CAPACITY))(route_ids.reshape(N_SP, SEQ_DEV, TOPK))
    group_ids = jnp.broadcast_to(jnp.arange(N_SP, dtype=jnp.int32)[:, None, None], slot_ids.shape)
    token_ids = group_ids * SEQ_DEV + jnp.broadcast_to(jnp.arange(SEQ_DEV, dtype=jnp.int32)[None, :, None], slot_ids.shape)
    table = jnp.full((N_SP, EXPERTS * CAPACITY), TOKENS, jnp.int32).at[group_ids, slot_ids].set(token_ids)
    table = jnp.transpose(table.reshape(N_SP, EXPERTS, CAPACITY), (1, 0, 2))
    padded = jnp.concatenate([normed, jnp.zeros((1, D), jnp.bfloat16)], axis=0)

    def run_expert(operands):
        gate_w, up_w, down_w, rows_index = operands
        gathered = padded[rows_index.reshape(-1)]
        hidden_part = (jax.nn.silu(jnp.dot(gathered, gate_w.T, preferred_element_type=jnp.float32)) * jnp.dot(gathered, up_w.T, preferred_element_type=jnp.float32)).astype(jnp.bfloat16)
        return jnp.dot(hidden_part, down_w, preferred_element_type=jnp.float32).astype(jnp.bfloat16)
    results = lax.map(run_expert, (expert_gate, expert_up, expert_down, table))
    results = results.reshape(EXPERTS * N_SP * CAPACITY, D)
    expert_of = slot_ids // CAPACITY
    position = slot_ids % CAPACITY
    flat_index = ((expert_of * N_SP + group_ids) * CAPACITY + position).astype(jnp.int32).reshape(TOKENS, TOPK)
    picked = results[flat_index].astype(jnp.float32)
    routed = lax.optimization_barrier(jnp.sum(picked * route_weights[:, :, None], axis=1))
    return (hidden_state.astype(jnp.float32) + shared_out + routed).astype(jnp.bfloat16)
```

```python
import jax
import jax.numpy as jnp
from jax import lax
from jax.sharding import PartitionSpec as P

epsilon = 1e-06
masked_score = -1e30
row_tile = 16


def rms_scale(values, gain_vec):
    squares = jnp.mean(values * values, axis=-1, keepdims=True)
    return values * lax.rsqrt(squares + epsilon) * gain_vec


def exchange(block, axis, offset):
    if offset == 0:
        return block
    size = lax.axis_size(axis)
    return lax.ppermute(block, axis, [(i, i ^ offset) for i in range(size)])


def tp_offsets():
    offsets = [0]
    bit = lax.axis_size("tp") // 2
    while bit:
        offsets = offsets + [offset ^ bit for offset in offsets]
        bit //= 2
    return offsets


def spread(block):
    blocks = [block]
    bit = lax.axis_size("tp") // 2
    while bit:
        blocks = blocks + [exchange(piece, "tp", bit) for piece in blocks]
        bit //= 2
    return blocks


def inner_size(size):
    inner = 1
    while (2 * inner) ** 2 <= size:
        inner *= 2
    return inner


def key_groups(key_rows, value_rows):
    size = lax.axis_size("sp")
    inner = inner_size(size)
    here = lax.axis_index("sp")
    chain = [(i, i + inner) for i in range(size - inner)]
    groups = []
    keys, values = key_rows, value_rows
    for step in range(size // inner):
        if step:
            keys = lax.ppermute(keys, "sp", chain)
            values = lax.ppermute(values, "sp", chain)
        source = here - step * inner
        groups.append(
            [
                (exchange(keys, "sp", j), exchange(values, "sp", j), source ^ j)
                for j in range(inner)
            ]
        )
    return groups


def attend(query_rows, key_rows, value_rows, map_weight, head_gain):
    seq_dev = query_rows.shape[0]
    heads_here = map_weight.shape[0]
    head_dim = head_gain.shape[0]
    half_dim = head_dim // 2
    score_scale = half_dim ** (-0.5)
    here = lax.axis_index("sp")
    steps = jnp.arange(seq_dev, dtype=jnp.int32)
    query_pos = here * seq_dev + steps
    query_heads = query_rows.reshape(seq_dev, heads_here, 2, half_dim)
    parts = []
    for step, group in enumerate(key_groups(key_rows, value_rows)):
        keys = jnp.concatenate([block[0] for block in group], axis=0)
        values = jnp.concatenate([block[1] for block in group], axis=0)
        key_heads = keys.reshape(-1, heads_here, 2, half_dim)
        value_heads = values.reshape(-1, heads_here, head_dim)
        scores = (
            jnp.einsum(
                "qhmd,khmd->hmqk", query_heads, key_heads, preferred_element_type=jnp.float32
            )
            * score_scale
        )
        if step == 0:
            key_pos = jnp.concatenate([block[2] * seq_dev + steps for block in group])
            scores = jnp.where(key_pos[None, :] <= query_pos[:, None], scores, masked_score)
        part_max = jnp.max(scores, axis=-1)
        expo = jnp.exp(scores - part_max[..., None])
        part_sum = jnp.sum(expo, axis=-1)
        product = jnp.einsum(
            "hmqk,khd->hmqd",
            expo.astype(jnp.bfloat16),
            value_heads,
            preferred_element_type=jnp.float32,
        )
        if step:
            part_max = jnp.where(group[0][2] >= 0, part_max, masked_score)
        parts.append((part_max, part_sum, product))
    row_max = parts[0][0]
    for part in parts[1:]:
        row_max = jnp.maximum(row_max, part[0])
    total = 0.0
    product = 0.0
    for part in parts:
        factor = jnp.exp(part[0] - row_max)
        total = total + factor * part[1]
        product = product + factor[..., None] * part[2]
    summed = product / total[..., None]
    diff_out = summed[:, 0] - map_weight[:, None, None] * summed[:, 1]
    head_out = rms_scale(diff_out, head_gain).astype(jnp.bfloat16)
    return jnp.transpose(head_out, (1, 0, 2)).reshape(seq_dev, heads_here * head_dim)


def body(
    residual_in,
    query_rows,
    key_rows,
    value_rows,
    map_weight,
    head_gain,
    out_proj,
    norm_gain,
    route_ids,
    route_weights,
    expert_gate,
    expert_up,
    expert_down,
    shared_gate,
    shared_up,
    shared_down,
):
    f32 = jnp.float32
    bf16 = jnp.bfloat16
    seq_dev, col_dev = residual_in.shape
    topk_count = route_ids.shape[1]
    sp_size = lax.axis_size("sp")
    hid_dev = expert_gate.shape[1]
    capacity = 5 * seq_dev * topk_count // (4 * sp_size)
    slots = -(-capacity // row_tile) * row_tile
    here = lax.axis_index("sp")
    tp_here = lax.axis_index("tp")
    offsets = tp_offsets()

    peers = here ^ jnp.arange(sp_size, dtype=jnp.int32)
    chosen = route_ids.T[None, :, :] == peers[:, None, None]
    named = jnp.any(chosen, axis=1)
    weight_of = jnp.sum(jnp.where(chosen, route_weights.T[None, :, :], 0.0), axis=1)
    rows = jnp.arange(seq_dev, dtype=jnp.int32)
    before = (rows[:, None] < rows[None, :]).astype(bf16)
    place = jnp.dot(named.astype(bf16), before, preferred_element_type=f32).astype(jnp.int32)
    place = jnp.where(named, place, -1)
    selected = place[:, None, :] == jnp.arange(slots, dtype=jnp.int32)[None, :, None]
    select = selected.astype(bf16).reshape(sp_size * slots, seq_dev)
    mix = jnp.where(selected, weight_of[:, None, :], 0.0).astype(bf16)

    def columns(weight, offset):
        return lax.dynamic_slice_in_dim(weight, (tp_here ^ offset) * col_dev, col_dev, 1)

    def hidden_rows(weight, offset):
        return lax.dynamic_slice_in_dim(weight, (tp_here ^ offset) * hid_dev, hid_dev, 0)

    gate_up = [
        jnp.concatenate([columns(expert_gate[0], o), columns(expert_up[0], o)], axis=0)
        for o in offsets
    ]
    down = [hidden_rows(expert_down[0], o) for o in offsets]
    down_shared = [hidden_rows(shared_down, o) for o in offsets]

    head_out = attend(query_rows, key_rows, value_rows, map_weight, head_gain)
    attn = jnp.dot(
        lax.all_gather(head_out, "tp", axis=1, tiled=True), out_proj, preferred_element_type=f32
    )
    hidden_state = (residual_in.astype(f32) + attn).astype(bf16)
    full_rows = lax.all_gather(hidden_state, "tp", axis=1, tiled=True)
    full_f32 = full_rows.astype(f32)
    inverse = lax.rsqrt(jnp.mean(full_f32 * full_f32, axis=-1, keepdims=True) + epsilon)
    normed = (full_f32 * inverse * norm_gain).astype(bf16)
    own_gain = lax.dynamic_slice_in_dim(norm_gain, tp_here * col_dev, col_dev, 0)
    own_cols = (hidden_state.astype(f32) * inverse * own_gain).astype(bf16)

    outgoing = jnp.dot(select, own_cols, preferred_element_type=f32).astype(bf16)
    outgoing = outgoing.reshape(sp_size, slots, col_dev)
    arrived = [exchange(outgoing[d], "sp", d) for d in range(sp_size)]

    cuts = [(0, sp_size // 2), (sp_size // 2, 3 * sp_size // 4), (3 * sp_size // 4, sp_size)]
    routed = 0.0
    gathered = []
    for first, last in cuts:
        gathered.append(spread(jnp.concatenate(arrived[first:last], axis=0)))

    shared_gate_part = lax.dot_general(
        normed, shared_gate, (((1,), (1,)), ((), ())), preferred_element_type=f32
    )
    shared_up_part = lax.dot_general(
        normed, shared_up, (((1,), (1,)), ((), ())), preferred_element_type=f32
    )
    shared_hidden = (jax.nn.silu(shared_gate_part) * shared_up_part).astype(bf16)
    base = hidden_state.astype(f32)

    for (first, last), blocks in zip(cuts, gathered):
        both = 0.0
        for block, weight in zip(blocks, gate_up):
            both = both + lax.dot_general(
                block, weight, (((1,), (1,)), ((), ())), preferred_element_type=f32
            )
        hidden = (jax.nn.silu(both[:, :hid_dev]) * both[:, hid_dev:]).astype(bf16)
        result = 0.0
        for block, weight in zip(spread(hidden), down):
            result = result + jnp.dot(block, weight, preferred_element_type=f32)
        result = result.astype(bf16).reshape(last - first, slots, col_dev)
        for d in range(first, last):
            returned = exchange(result[d - first], "sp", d)
            routed = routed + lax.dot_general(
                mix[d], returned, (((0,), (0,)), ((), ())), preferred_element_type=f32
            )
    for block, weight in zip(spread(shared_hidden), down_shared):
        base = base + jnp.dot(block, weight, preferred_element_type=f32)
    return (base + routed).astype(bf16)


def solution(mesh):
    in_specs = (
        P("sp", "tp"),
        P("sp", "tp"),
        P("sp", "tp"),
        P("sp", "tp"),
        P("tp"),
        P(),
        P(None, "tp"),
        P(),
        P("sp", None),
        P("sp", None),
        P("sp", "tp", None),
        P("sp", "tp", None),
        P("sp", None, "tp"),
        P("tp", None),
        P("tp", None),
        P(None, "tp"),
    )
    out_specs = P("sp", "tp")
    return jax.shard_map(body, mesh=mesh, in_specs=in_specs, out_specs=out_specs, check_vma=False)
```

```python
import functools
import jax
import jax.numpy as jnp
from jax import lax
from jax.experimental import pallas as pl
from jax.experimental.pallas import tpu as pltpu
from jax.sharding import PartitionSpec as P

epsilon = 1e-06
masked_score = -1e30
row_tile = 16


def rms_scale(values, gain_vec):
    squares = jnp.mean(values * values, axis=-1, keepdims=True)
    return values * lax.rsqrt(squares + epsilon) * gain_vec


def exchange(block, axis, offset):
    if offset == 0:
        return block
    size = lax.axis_size(axis)
    return lax.ppermute(block, axis, [(i, i ^ offset) for i in range(size)])


def tp_offsets():
    offsets = [0]
    bit = lax.axis_size("tp") // 2
    while bit:
        offsets = offsets + [offset ^ bit for offset in offsets]
        bit //= 2
    return offsets


def spread(block):
    blocks = [block]
    bit = lax.axis_size("tp") // 2
    while bit:
        blocks = blocks + [exchange(piece, "tp", bit) for piece in blocks]
        bit //= 2
    return blocks


def inner_size(size):
    inner = 1
    while (2 * inner) ** 2 <= size:
        inner *= 2
    return inner


def key_groups(both_rows):
    size = lax.axis_size("sp")
    inner = inner_size(size)
    chain = [(i, i + inner) for i in range(size - inner)]
    groups = []
    for step in range(size // inner):
        if step:
            both_rows = lax.ppermute(both_rows, "sp", chain)
        groups.append((step, [exchange(both_rows, "sp", j) for j in range(inner)]))
    return groups


def attend_kernel(
    steps, inner, head_dim, first, last, here_ref, weight_ref, gain_ref, query_ref, *refs
):
    count = len(steps) * inner
    block_refs, refs = refs[:count], refs[count:]
    seq_dev, width = query_ref.shape
    half_dim = head_dim // 2
    band = min(128, width)
    heads = band // head_dim
    pairs = 2 * heads
    score_scale = half_dim ** (-0.5)
    here = here_ref[0]
    if not first:
        old_refs, refs = refs[:3], refs[3:]
    lane = lax.broadcasted_iota(jnp.int32, (seq_dev, band), 1)
    query_pos = lax.broadcasted_iota(jnp.int32, (seq_dev, seq_dev), 0)
    key_pos = lax.broadcasted_iota(jnp.int32, (seq_dev, seq_dev), 1)
    ahead = query_pos - key_pos
    for number in range(width // band):
        left = number * band
        query = query_ref[:, left : left + band].astype(jnp.float32)
        stacked = jnp.concatenate(
            [
                jnp.where(lane // half_dim == pair, query, 0.0).astype(jnp.bfloat16)
                for pair in range(pairs)
            ],
            axis=0,
        )
        if first:
            row_max = total = product = None
        else:
            row_max, total, product = [ref[number] for ref in old_refs]
        for place, step in enumerate(steps):
            scores = []
            for j in range(inner):
                keys = block_refs[place * inner + j][:, left : left + band]
                score = (
                    lax.dot_general(
                        stacked, keys, (((1,), (1,)), ((), ())), preferred_element_type=jnp.float32
                    )
                    * score_scale
                )
                source = (here - step * inner) ^ j
                behind = jnp.where(source >= 0, here - source, -(2**12)) * seq_dev
                bias = jnp.where(ahead + behind >= 0, 0.0, masked_score)
                scores.append(score + jnp.concatenate([bias] * pairs, axis=0))
            new_max = functools.reduce(
                jnp.maximum, [jnp.max(score, axis=1, keepdims=True) for score in scores]
            )
            if row_max is not None:
                new_max = jnp.maximum(row_max, new_max)
                factor = jnp.exp(row_max - new_max)
                total, product = total * factor, product * factor
            for j in range(inner):
                values = block_refs[place * inner + j][:, width + left : width + left + band]
                expo = jnp.exp(scores[j] - new_max)
                part = jnp.sum(expo, axis=1, keepdims=True)
                piece = jnp.dot(
                    expo.astype(jnp.bfloat16), values, preferred_element_type=jnp.float32
                )
                if row_max is None and j == 0:
                    total, product = part, piece
                else:
                    total, product = total + part, product + piece
            row_max = new_max
        if not last:
            for ref, value in zip(refs, (row_max, total, product)):
                ref[number] = value
            continue
        summed = product / total
        out = jnp.zeros((seq_dev, band), jnp.float32)
        for head in range(heads):
            maps = [
                summed[pair * seq_dev : (pair + 1) * seq_dev] for pair in (2 * head, 2 * head + 1)
            ]
            diff_out = maps[0] - weight_ref[number * heads + head] * maps[1]
            mine = lane // head_dim == head
            squares = jnp.sum(jnp.where(mine, diff_out * diff_out, 0.0), axis=1, keepdims=True)
            scaled = diff_out * lax.rsqrt(squares / head_dim + epsilon)
            out = jnp.where(mine, scaled, out)
        refs[0][:, left : left + band] = (out * gain_ref[:, :band]).astype(jnp.bfloat16)


def attend(query_rows, key_rows, value_rows, map_weight, head_gain):
    seq_dev, width = query_rows.shape
    head_dim = head_gain.shape[0]
    band = min(128, width)
    bands = width // band
    pair_rows = 2 * (band // head_dim) * seq_dev
    here = jnp.full((1,), lax.axis_index("sp"), jnp.int32)
    gain = jnp.tile(head_gain, band // head_dim)[None, :]
    groups = key_groups(jnp.concatenate([key_rows, value_rows], axis=1))
    inner = len(groups[0][1])
    state_shapes = [
        jax.ShapeDtypeStruct((bands, pair_rows, columns), jnp.float32) for columns in (1, 1, band)
    ]
    vmem = pl.BlockSpec(memory_space=pltpu.VMEM)
    smem = pl.BlockSpec(memory_space=pltpu.SMEM)
    state = ()
    for cut in (groups[:-1], groups[-1:]):
        last = cut[-1] is groups[-1]
        blocks = [block for _, group in cut for block in group]
        kernel = functools.partial(
            attend_kernel, [step for step, _ in cut], inner, head_dim, not state, last
        )
        state = pl.pallas_call(
            kernel,
            out_shape=jax.ShapeDtypeStruct((seq_dev, width), jnp.bfloat16) if last else state_shapes,
            in_specs=[smem, smem] + [vmem] * (2 + len(blocks) + len(state)),
            out_specs=vmem if last else [vmem] * 3,
            name="attend_last" if last else "attend_first",
        )(here, map_weight, gain, query_rows, *blocks, *state)
    return state


def body(
    residual_in,
    query_rows,
    key_rows,
    value_rows,
    map_weight,
    head_gain,
    out_proj,
    norm_gain,
    route_ids,
    route_weights,
    expert_gate,
    expert_up,
    expert_down,
    shared_gate,
    shared_up,
    shared_down,
):
    f32 = jnp.float32
    bf16 = jnp.bfloat16
    seq_dev, col_dev = residual_in.shape
    topk_count = route_ids.shape[1]
    sp_size = lax.axis_size("sp")
    hid_dev = expert_gate.shape[1]
    capacity = 5 * seq_dev * topk_count // (4 * sp_size)
    slots = -(-capacity // row_tile) * row_tile
    here = lax.axis_index("sp")
    tp_here = lax.axis_index("tp")
    offsets = tp_offsets()

    peers = here ^ jnp.arange(sp_size, dtype=jnp.int32)
    chosen = route_ids.T[None, :, :] == peers[:, None, None]
    named = jnp.any(chosen, axis=1)
    weight_of = jnp.sum(jnp.where(chosen, route_weights.T[None, :, :], 0.0), axis=1)
    rows = jnp.arange(seq_dev, dtype=jnp.int32)
    before = (rows[:, None] < rows[None, :]).astype(bf16)
    place = jnp.dot(named.astype(bf16), before, preferred_element_type=f32).astype(jnp.int32)
    place = jnp.where(named, place, -1)
    selected = place[:, None, :] == jnp.arange(slots, dtype=jnp.int32)[None, :, None]
    select = selected.astype(bf16).reshape(sp_size * slots, seq_dev)
    mix = jnp.where(selected, weight_of[:, None, :], 0.0).astype(bf16)

    def columns(weight, offset):
        return lax.dynamic_slice_in_dim(weight, (tp_here ^ offset) * col_dev, col_dev, 1)

    def hidden_rows(weight, offset):
        return lax.dynamic_slice_in_dim(weight, (tp_here ^ offset) * hid_dev, hid_dev, 0)

    gate_up = [
        jnp.concatenate([columns(expert_gate[0], o), columns(expert_up[0], o)], axis=0)
        for o in offsets
    ]
    down = [hidden_rows(expert_down[0], o) for o in offsets]
    down_shared = [hidden_rows(shared_down, o) for o in offsets]

    head_out = attend(query_rows, key_rows, value_rows, map_weight, head_gain)
    attn = jnp.dot(
        lax.all_gather(head_out, "tp", axis=1, tiled=True), out_proj, preferred_element_type=f32
    )
    hidden_state = (residual_in.astype(f32) + attn).astype(bf16)
    full_rows = lax.all_gather(hidden_state, "tp", axis=1, tiled=True)
    full_f32 = full_rows.astype(f32)
    inverse = lax.rsqrt(jnp.mean(full_f32 * full_f32, axis=-1, keepdims=True) + epsilon)
    normed = (full_f32 * inverse * norm_gain).astype(bf16)
    own_gain = lax.dynamic_slice_in_dim(norm_gain, tp_here * col_dev, col_dev, 0)
    own_cols = (hidden_state.astype(f32) * inverse * own_gain).astype(bf16)

    outgoing = jnp.dot(select, own_cols, preferred_element_type=f32).astype(bf16)
    outgoing = outgoing.reshape(sp_size, slots, col_dev)
    order = [*range(sp_size // 2, sp_size), *range(sp_size // 2)]
    arrived = {d: exchange(outgoing[d], "sp", d) for d in order}

    cuts = [(sp_size // 2, 3 * sp_size // 4), (3 * sp_size // 4, sp_size), (0, sp_size // 2)]
    routed = 0.0
    gathered = []
    for first, last in cuts:
        gathered.append(spread(jnp.concatenate([arrived[d] for d in range(first, last)], axis=0)))

    shared_gate_part = lax.dot_general(
        normed, shared_gate, (((1,), (1,)), ((), ())), preferred_element_type=f32
    )
    shared_up_part = lax.dot_general(
        normed, shared_up, (((1,), (1,)), ((), ())), preferred_element_type=f32
    )
    shared_hidden = (jax.nn.silu(shared_gate_part) * shared_up_part).astype(bf16)
    base = hidden_state.astype(f32)

    for (first, last), blocks in zip(cuts, gathered):
        both = 0.0
        for block, weight in zip(blocks, gate_up):
            both = both + lax.dot_general(
                block, weight, (((1,), (1,)), ((), ())), preferred_element_type=f32
            )
        hidden = (jax.nn.silu(both[:, :hid_dev]) * both[:, hid_dev:]).astype(bf16)
        result = 0.0
        for block, weight in zip(spread(hidden), down):
            result = result + jnp.dot(block, weight, preferred_element_type=f32)
        result = result.astype(bf16).reshape(last - first, slots, col_dev)
        for d in range(first, last):
            returned = exchange(result[d - first], "sp", d)
            routed = routed + lax.dot_general(
                mix[d], returned, (((0,), (0,)), ((), ())), preferred_element_type=f32
            )
    for block, weight in zip(spread(shared_hidden), down_shared):
        base = base + jnp.dot(block, weight, preferred_element_type=f32)
    return (base + routed).astype(bf16)


def solution(mesh):
    in_specs = (
        P("sp", "tp"),
        P("sp", "tp"),
        P("sp", "tp"),
        P("sp", "tp"),
        P("tp"),
        P(),
        P(None, "tp"),
        P(),
        P("sp", None),
        P("sp", None),
        P("sp", "tp", None),
        P("sp", "tp", None),
        P("sp", None, "tp"),
        P("tp", None),
        P("tp", None),
        P(None, "tp"),
    )
    out_specs = P("sp", "tp")
    return jax.shard_map(body, mesh=mesh, in_specs=in_specs, out_specs=out_specs, check_vma=False)
```
